32 devices in a mesh: sp: 16 (over z, y, x), tp: 2 (over core).
Axes of the slice: x: 2, y: 2, z: 4, core: 2. Of those that a mesh axis runs over, the one named last changes fastest.
Arguments:
- tokens: bfloat16 [4096, 4096], P('sp'), may hold values from -5 to 5
- documents: int32 [4096], P('sp'), may hold values from 0 to 3, never falling along the last dimension, each value on 1 to 2048 neighbouring positions
- norm_gain: float32 [2, 4096], replicated, may hold values from 0.1 to 1.9
- in_weight: bfloat16 [2, 4096, 2048], P(None, 'sp', 'tp'), may hold values from -0.09375 to 0.09375
- conv_taps: float32 [2, 4, 2048], P(None, None, 'tp'), may hold values from -3 to 3
- conv_bias: float32 [2, 2048], P(None, 'tp'), may hold values from -0.75 to 0.75
- recur_gate: bfloat16 [2, 32, 64, 64], P(None, 'tp'), may hold values from -0.75 to 0.75
- input_gate: bfloat16 [2, 32, 64, 64], P(None, 'tp'), may hold values from -0.75 to 0.75
- recur_bias: float32 [2, 2048], P(None, 'tp'), may hold values from -4 to 4
- input_bias: float32 [2, 2048], P(None, 'tp'), may hold values from -4 to 4
- decay_param: float32 [2, 2048], P(None, 'tp'), may hold values from 4 to 7
- out_weight: bfloat16 [2, 2048, 4096], P(None, 'tp', 'sp'), may hold values from -0.375 to 0.375
Outputs:
- layered: bfloat16 [4096, 4096], P('sp')
The draws below stay inside these ranges and needn't reach their ends.
All inputs are finite; a program needn't handle non-finite values.
Results may differ from the reference program's by a relative error of at most 0.017.
Values may be sent and summed in bfloat16 or wider, within the bound.
A program may use at most 128 MiB of HBM per device.

```python
import math
import jax
import jax.numpy as jnp
import numpy as np
from jax import lax

D = 4096
RW = 2048
BD = 64
K = 4
LAYERS = 2
TOK_DEV = 256
TOKENS = 4096
NB = 32
N_SP = 16
N_TP = 2


def draw_tokens(key, part):
    scale_key, value_key, mean_key = jax.random.split(jax.random.fold_in(key, 11), 3)
    log_scale = jax.random.uniform(scale_key, (TOKENS // 128, 1), jnp.float32, -1.3863, -0.2877)
    block_scale = jnp.repeat(jnp.exp(log_scale), 128, axis=0)
    base = jax.random.normal(value_key, (TOKENS, D), jnp.float32)
    base = jnp.clip(base, -6.0, 6.0)
    return (base * block_scale).astype(jnp.bfloat16)


def draw_decay_param(key, part):
    flag_key, slow_key, fast_key = jax.random.split(jax.random.fold_in(key, 23), 3)
    picked = jax.random.randint(flag_key, (LAYERS, RW), 0, 2)
    slow_value = jax.random.uniform(slow_key, (LAYERS, RW), jnp.float32, 6.5, 7.0)
    fast_value = jax.random.uniform(fast_key, (LAYERS, RW), jnp.float32, 4.0, 5.0)
    return jnp.where(picked == 0, fast_value, slow_value)


def shard_levels(own_key, extent, pieces, smallest, high):
    gain = 1.0
    for dim, parts in pieces:
        draws = jax.random.uniform(jax.random.fold_in(jax.random.fold_in(own_key, 6), dim), (parts,), jnp.float32, smallest / len(pieces), high / len(pieces))
        gain = gain * jnp.repeat(jnp.exp(draws), extent[dim] // parts).reshape((-1,) + (1,) * (len(extent) - 1 - dim))
    return gain


def split_up(number_of, total, bound, lean):
    portions = [(1 << 20) // math.isqrt(standing ** lean) + 1 for standing in range(2, number_of + 1)]
    surplus, holding = total - bound - (number_of - 1), [1] * (number_of - 1)
    while surplus > 0:
        movable = [i for i in range(number_of - 1) if holding[i] < bound]
        mass, budget = sum([portions[i] for i in movable]), surplus
        for i in movable:
            addition = min(bound - holding[i], max(1, budget * portions[i] // mass), surplus)
            holding[i] = holding[i] + addition
            surplus = surplus - addition
    return np.array([bound] + holding)


def ragged(rng, number_of, total, most, slope):
    if number_of == 2:
        one = jax.random.randint(rng, (), max(1, total - most), min(most, total - 1) + 1)
        return jnp.stack([one, total - one])
    lengths = jnp.asarray(split_up(number_of, total, most, slope), jnp.int32)
    twos = (number_of - 1) // 2
    donor, sink = lengths[1:1 + 2 * twos:2], lengths[2:2 + 2 * twos:2]
    margin = jnp.minimum(donor - 1, most - sink)
    moved = jax.random.randint(jax.random.fold_in(rng, 1), (twos,), 0, 1 << 20) % (margin + 1)
    lengths = lengths.at[1:1 + 2 * twos:2].set(donor - moved).at[2:2 + 2 * twos:2].set(sink + moved)
    return lengths[jax.random.permutation(jax.random.fold_in(rng, 2), number_of)]


def bell_draw(rng, shape, scale, most, shards=(), kind=jnp.bfloat16):
    drawn = jax.random.normal(rng, shape, jnp.float32) * scale
    if len(shards) > 0:
        drawn = shard_levels(rng, shape, shards, -0.22, 0.18) * drawn
    return jnp.clip(drawn, min=-most, max=most).astype(kind)


def setup_inputs(seed: int = 0) -> dict:
    splits = jax.random.split(jax.random.key(seed), 13)
    tokens = draw_tokens(jax.random.fold_in(splits[12], 71), 0)
    documents = jnp.searchsorted(jnp.cumsum(ragged(splits[1], N_SP // 4, TOKENS, 8 * TOK_DEV, 0)), jnp.arange(TOKENS), side="right").astype(jnp.int32)
    norm_gain = jnp.clip(1.0 + 0.18 * jax.random.normal(splits[2], (LAYERS, D), jnp.float32), 0.1, 1.9)
    in_weight = bell_draw(splits[3], (LAYERS, D, RW), D ** -0.5, 0.09375, ((1, 16), (2, 2)))
    conv_taps = bell_draw(splits[4], (LAYERS, K, RW), K ** -0.5, 3.0, ((2, 2),), jnp.float32)
    conv_bias = bell_draw(splits[5], (LAYERS, RW), 0.05, 0.75, ((1, 2),), jnp.float32)
    recur_gate = bell_draw(splits[6], (LAYERS, NB, BD, BD), BD ** -0.5, 0.75, ((1, 2),))
    input_gate = bell_draw(splits[7], (LAYERS, NB, BD, BD), BD ** -0.5, 0.75, ((1, 2),))
    recur_bias = bell_draw(splits[8], (LAYERS, RW), 1.0, 4.0, ((1, 2),), jnp.float32)
    input_bias = bell_draw(splits[9], (LAYERS, RW), 1.0, 4.0, ((1, 2),), jnp.float32)
    decay_param = draw_decay_param(jax.random.fold_in(splits[12], 71), 0)
    out_weight = bell_draw(splits[11], (LAYERS, RW, D), (RW // 8) ** -0.5, 0.375, ((1, 2), (2, 16)))
    return {"tokens": tokens, "documents": documents, "norm_gain": norm_gain, "in_weight": in_weight, "conv_taps": conv_taps, "conv_bias": conv_bias, "recur_gate": recur_gate, "input_gate": input_gate, "recur_bias": recur_bias, "input_bias": input_bias, "decay_param": decay_param, "out_weight": out_weight}


RG_C = 8.0
EPS = 0.1

def norm_rows(values_in, gain_row):
    values = values_in.astype(jnp.float32)
    scaled = values * lax.rsqrt(lax.optimization_barrier(jnp.mean(values * values, axis=-1, keepdims=True)) + EPS)
    return (scaled * gain_row[None, :]).astype(jnp.bfloat16)

def combine(earlier, following):
    return (earlier[0] * following[0], following[0] * earlier[1] + following[1])

def reference(tokens, documents, norm_gain, in_weight, conv_taps, conv_bias, recur_gate, input_gate, recur_bias, input_bias, decay_param, out_weight):
    state_x = tokens
    prev_doc = jnp.concatenate([documents[:1], documents[:-1]])
    reset = documents != prev_doc
    group_width = RW // N_TP
    for depth_at in range(LAYERS):
        normed = norm_rows(state_x, norm_gain[depth_at])
        mixed_in = jnp.dot(normed, in_weight[depth_at], preferred_element_type=jnp.float32).astype(jnp.bfloat16)
        values_in = mixed_in.astype(jnp.float32)
        conv_sum = conv_bias[depth_at][None, :] + conv_taps[depth_at, 0][None, :] * values_in
        for lag_step in range(1, K):
            shifted = jnp.concatenate([jnp.zeros((lag_step, RW), jnp.float32), values_in[:-lag_step]], axis=0)
            shifted_doc = jnp.concatenate([jnp.full((lag_step,), -1, jnp.int32), documents[:-lag_step]], axis=0)
            same_doc = (shifted_doc == documents)[:, None]
            conv_sum = conv_sum + jnp.where(same_doc, conv_taps[depth_at, lag_step][None, :] * shifted, 0.0)
        conv_out = conv_sum.astype(jnp.bfloat16)
        grouped = conv_out.astype(jnp.float32).reshape(TOKENS, NB, BD)
        recur_rate = jax.nn.sigmoid(jnp.einsum('snb,nbc->snc', grouped, recur_gate[depth_at].astype(jnp.float32)).reshape(TOKENS, RW) + recur_bias[depth_at][None, :])
        input_rate = jax.nn.sigmoid(jnp.einsum('snb,nbc->snc', grouped, input_gate[depth_at].astype(jnp.float32)).reshape(TOKENS, RW) + input_bias[depth_at][None, :])
        log_decay = -RG_C * jax.nn.softplus(-decay_param[depth_at])[None, :] * recur_rate
        decay_now = jnp.where(reset[:, None], 0.0, jnp.exp(log_decay))
        drive_term = jnp.sqrt(jnp.maximum(-jnp.expm1(2.0 * log_decay), 0.0)) * (input_rate * conv_out.astype(jnp.float32))
        _, states = lax.associative_scan(combine, (decay_now, drive_term), axis=0)
        hidden = states.astype(jnp.bfloat16)
        summed = jnp.zeros((TOKENS, D), jnp.float32)
        for group in range(N_TP):
            low = group * group_width
            partial_term = jnp.dot(hidden[:, low:low + group_width], out_weight[depth_at, low:low + group_width], preferred_element_type=jnp.float32).astype(jnp.bfloat16)
            partial_term = lax.optimization_barrier(partial_term)
            summed = summed + partial_term.astype(jnp.float32)
        state_x = (state_x.astype(jnp.float32) + summed).astype(jnp.bfloat16)
    return state_x
```

```python
import functools

import jax
import jax.numpy as jnp
from jax import lax
from jax.experimental import pallas as pl
from jax.experimental.pallas import tpu as pltpu
from jax.sharding import PartitionSpec as P

RG_C = 8.0
EPS = 0.1
MESH = pl.DeviceIdType.MESH
F32 = jnp.float32
BF16 = jnp.bfloat16
VM = pl.BlockSpec(memory_space=pltpu.VMEM)


def send(src, dst, send_sem, recv_sem, **device):
    return pltpu.make_async_remote_copy(
        src_ref=src,
        dst_ref=dst,
        send_sem=send_sem,
        recv_sem=recv_sem,
        device_id=device,
        device_id_type=MESH,
    )


def swap_kernel(g, x_ref, o_ref, send_sem, recv_sem, own_sem):
    me = lax.axis_index("sp")
    inner, base = lax.rem(me, g), me - lax.rem(me, g)
    own = pltpu.make_async_copy(x_ref.at[inner], o_ref.at[inner], own_sem)
    own.start()

    def go(step, _):
        j = lax.rem(inner + step, g)
        send(x_ref.at[j], o_ref.at[inner], send_sem.at[j], recv_sem.at[inner], sp=base + j).start()
        return 0

    lax.fori_loop(1, g, go, 0)

    def done(step, _):
        j = lax.rem(inner + step, g)
        copy = send(x_ref.at[j], o_ref.at[j], send_sem.at[j], recv_sem.at[j], sp=base + j)
        copy.wait_recv()
        copy.wait_send()
        return 0

    lax.fori_loop(1, g, done, 0)
    own.wait()


def swapped(x, g):
    return pl.pallas_call(
        functools.partial(swap_kernel, g),
        out_shape=jax.ShapeDtypeStruct(x.shape, x.dtype),
        in_specs=[pl.BlockSpec(memory_space=pl.ANY)],
        out_specs=pl.BlockSpec(memory_space=pl.ANY),
        scratch_shapes=[
            pltpu.SemaphoreType.DMA((g,)),
            pltpu.SemaphoreType.DMA((g,)),
            pltpu.SemaphoreType.DMA,
        ],
        compiler_params=pltpu.CompilerParams(has_side_effects=True),
    )(x)


def minus_expm1(x):
    series = 1.0 + x * (1.0 / 8.0)
    for n in range(7, 1, -1):
        series = 1.0 + (x * (1.0 / n)) * series
    return jnp.where(x > -0.5, -x * series, 1.0 - jnp.exp(x))


def layer_kernel(
    g, n_sp, n_tp, taps, feature_count,
    x_ref, gain_ref, win_ref, wout_ref, vec_ref, mask_ref, gate_ref,
    o_ref,
    part, gotten, tails, tail_out, ext, a_buf, b_buf, ends, hid, psend, pgot,
    rs_send, rs_recv, tail_sem, end_send, end_recv, ag_send, ag_recv, tp_send, tp_recv,
):
    me = lax.axis_index("sp")
    core = lax.axis_index("tp")
    inner, base = lax.rem(me, g), me - lax.rem(me, g)
    rows = x_ref.shape[1]
    chans = win_ref.shape[1]
    sub = rows // 8

    def project(step, _):
        j = lax.rem(inner + step, g)
        x = x_ref[j].astype(F32)
        squares = jnp.sum(x * x, axis=1, keepdims=True)
        high = squares.astype(BF16).astype(F32)
        lane = lax.broadcasted_iota(jnp.int32, (rows, 128), 1)
        extra = jnp.where(lane == 0, high, jnp.where(lane == 1, squares - high, 0.0))
        scaled = (x * gain_ref[...]).astype(BF16)
        out = jnp.dot(scaled, win_ref[...], preferred_element_type=F32)
        part[j, :, :chans] = out.astype(BF16)
        part[j, :, chans:] = extra.astype(BF16)

        @pl.when(step < g)
        def _():
            send(
                part.at[j], gotten.at[inner], rs_send.at[j], rs_recv.at[inner], sp=base + j
            ).start()

        return 0

    lax.fori_loop(1, g + 1, project, 0)
    ext[pl.ds(8, rows), :] = part[inner, :, :chans].astype(F32)
    sums = part[inner, :, chans:].astype(F32)

    def collect(step, sums):
        j = lax.rem(inner + step, g)
        send(part.at[j], gotten.at[j], rs_send.at[j], rs_recv.at[j], sp=base + j).wait_recv()
        ext[pl.ds(8, rows), :] += gotten[j, :, :chans].astype(F32)
        return sums + gotten[j, :, chans:].astype(F32)

    sums = lax.fori_loop(1, g, collect, sums)
    total = jnp.sum(sums, axis=1, keepdims=True)
    scale = lax.rsqrt(total * (1.0 / feature_count) + EPS)
    mixed = (ext[pl.ds(8, rows), :] * scale).astype(BF16)
    tail_out[...] = mixed[rows - 16 :]

    after = lax.rem(me + 1, n_sp)

    tail_copy = send(tail_out, tails, tail_sem.at[0], tail_sem.at[1], sp=after)

    tail_copy.start()
    ext[pl.ds(8, rows), :] = mixed.astype(F32)
    tail_copy.wait_recv()
    ext[pl.ds(0, 8), :] = tails[8:].astype(F32)

    pair = gate_ref.shape[1]
    for col in range(0, chans, pair):
        cols = pl.ds(col, pair)
        conv = vec_ref[pl.ds(taps, 1), cols] + vec_ref[pl.ds(0, 1), cols] * ext[pl.ds(8, rows), cols]
        for lag in range(1, taps):
            shifted = ext[pl.ds(8 - lag, rows), cols]
            same = mask_ref[:, lag : lag + 1] > 0.5
            conv = conv + jnp.where(same, vec_ref[pl.ds(lag, 1), cols] * shifted, 0.0)
        conv_out = conv.astype(BF16)
        both = jnp.dot(conv_out, gate_ref[col // pair], preferred_element_type=F32)
        recur = jax.nn.sigmoid(both[:, :pair] + vec_ref[pl.ds(taps + 1, 1), cols])
        inp = jax.nn.sigmoid(both[:, pair:] + vec_ref[pl.ds(taps + 2, 1), cols])
        log_decay = vec_ref[pl.ds(taps + 3, 1), cols] * recur
        keep = mask_ref[:, 0:1] > 0.5
        a_buf[col // pair] = jnp.where(keep, jnp.exp(log_decay), 0.0)
        b_buf[col // pair] = jnp.sqrt(jnp.maximum(minus_expm1(2.0 * log_decay), 0.0)) * (
            inp * conv_out.astype(F32)
        )

    lanes = a_buf.shape[0]

    def advance(r, carry):
        at = pl.ds(r, 8, stride=sub)
        following = []
        for c in range(lanes):
            decay, state = carry[c]
            a = a_buf[c, at, :]
            decay = decay * a
            state = a * state + b_buf[c, at, :]
            a_buf[c, at, :] = decay
            b_buf[c, at, :] = state
            following.append((decay, state))
        return tuple(following)

    start = (jnp.ones((8, pair), F32), jnp.zeros((8, pair), F32))
    chunks = lax.fori_loop(0, sub, advance, (start,) * lanes, unroll=2)
    decay = jnp.concatenate([c[0] for c in chunks], axis=1)
    state = jnp.concatenate([c[1] for c in chunks], axis=1)
    prefix = [(jnp.ones((1, chans), F32), jnp.zeros((1, chans), F32))]
    for s in range(8):
        d, h = prefix[-1]
        prefix.append((d * decay[s : s + 1], decay[s : s + 1] * h + state[s : s + 1]))
    ends[me, 0:1, :] = prefix[8][0]
    ends[me, 1:2, :] = prefix[8][1]

    def end_to(dst, _):
        @pl.when(dst > me)
        def _():
            send(ends.at[me], ends.at[me], end_send.at[dst], end_recv.at[me], sp=dst).start()

        return 0

    lax.fori_loop(0, n_sp, end_to, 0)

    def fold(src, state):
        @pl.when(src < me)
        def _():
            send(ends.at[src], ends.at[src], end_send.at[src], end_recv.at[src], sp=src).wait_recv()

        return jnp.where(src < me, ends[src, 0:1, :] * state + ends[src, 1:2, :], state)

    carried = lax.fori_loop(0, n_sp, fold, jnp.zeros((1, chans), F32))
    for s in range(8):
        at = pl.ds(s * sub, sub)
        enter = prefix[s][0] * carried + prefix[s][1]
        for c in range(lanes):
            cols = pl.ds(c * pair, pair)
            one = enter[:, c * pair : (c + 1) * pair]
            hid[inner, at, cols] = (b_buf[c, at, :] + a_buf[c, at, :] * one).astype(BF16)

    def spread(step, _):
        j = lax.rem(inner + step, g)
        send(hid.at[inner], hid.at[inner], ag_send.at[j], ag_recv.at[inner], sp=base + j).start()
        return 0

    lax.fori_loop(1, g, spread, 0)

    blocks, width = wout_ref.shape[0], wout_ref.shape[2]

    def unproject(step, _):
        j = lax.rem(inner + step, g)

        @pl.when(step > 0)
        def _():
            send(hid.at[j], hid.at[j], ag_send.at[j], ag_recv.at[j], sp=base + j).wait_recv()

        h = hid[j]
        for block in range(blocks):
            out = jnp.dot(h, wout_ref[block], preferred_element_type=F32)
            psend[j, :, block * width : (block + 1) * width] = out.astype(BF16)
        for other in range(1, n_tp):
            peer = lax.rem(core + other, n_tp)
            send(
                psend.at[j], pgot.at[core, j], tp_send.at[peer, j], tp_recv.at[core, j], tp=peer
            ).start()
        return 0

    lax.fori_loop(0, g, unproject, 0)

    def finish(step, _):
        j = lax.rem(inner + step, g)
        summed = psend[j].astype(F32)
        for other in range(1, n_tp):
            peer = lax.rem(core + other, n_tp)
            copy = send(
                psend.at[j], pgot.at[peer, j], tp_send.at[peer, j], tp_recv.at[peer, j], tp=peer
            )
            copy.wait_recv()
            summed = summed + pgot[peer, j].astype(F32)
            copy.wait_send()
        o_ref[j] = (x_ref[j].astype(F32) + summed).astype(BF16)
        return 0

    lax.fori_loop(0, g, finish, 0)

    def close(step, _):
        j = lax.rem(inner + step, g)
        send(part.at[j], gotten.at[j], rs_send.at[j], rs_recv.at[j], sp=base + j).wait_send()
        send(hid.at[inner], hid.at[j], ag_send.at[j], ag_recv.at[j], sp=base + j).wait_send()
        return 0

    lax.fori_loop(1, g, close, 0)
    tail_copy.wait_send()

    def end_close(dst, _):
        @pl.when(dst > me)
        def _():
            send(ends.at[me], ends.at[me], end_send.at[dst], end_recv.at[me], sp=dst).wait_send()

        return 0

    lax.fori_loop(0, n_sp, end_close, 0)


def one_layer(g, n_sp, n_tp, taps, x, gain, win, wout, vec, mask, gates, features):
    rows, part_width = x.shape[1], x.shape[2]
    chans = win.shape[1]
    dma = pltpu.SemaphoreType.DMA
    return pl.pallas_call(
        functools.partial(layer_kernel, g, n_sp, n_tp, taps, features),
        out_shape=jax.ShapeDtypeStruct(x.shape, x.dtype),
        in_specs=[VM] * 7,
        out_specs=VM,
        scratch_shapes=[
            pltpu.VMEM((g, rows, chans + 128), BF16),
            pltpu.VMEM((g, rows, chans + 128), BF16),
            pltpu.VMEM((16, chans), BF16),
            pltpu.VMEM((16, chans), BF16),
            pltpu.VMEM((rows + 8, chans), F32),
            pltpu.VMEM((chans // 128, rows, 128), F32),
            pltpu.VMEM((chans // 128, rows, 128), F32),
            pltpu.VMEM((n_sp, 2, chans), F32),
            pltpu.VMEM((g, rows, chans), BF16),
            pltpu.VMEM((g, rows, part_width), BF16),
            pltpu.VMEM((n_tp, g, rows, part_width), BF16),
            dma((g,)),
            dma((g,)),
            dma((2,)),
            dma((n_sp,)),
            dma((n_sp,)),
            dma((g,)),
            dma((g,)),
            dma((n_tp, g)),
            dma((n_tp, g)),
        ],
        compiler_params=pltpu.CompilerParams(
            has_side_effects=True, vmem_limit_bytes=60 * 1024 * 1024
        ),
        cost_estimate=pl.CostEstimate(
            flops=100_000_000_000, bytes_accessed=100_000_000, transcendentals=0
        ),
    )(x, gain, win, wout, vec, mask, gates)


def per_device(
    g,
    tokens,
    documents,
    norm_gain,
    in_weight,
    conv_taps,
    conv_bias,
    recur_gate,
    input_gate,
    recur_bias,
    input_bias,
    decay_param,
    out_weight,
):
    n_sp, n_tp = lax.axis_size("sp"), lax.axis_size("tp")
    outer = n_sp // g
    rows, features = tokens.shape
    layers, block_width, chans = in_weight.shape
    taps = conv_taps.shape[1]
    me = lax.axis_index("sp")
    inner = lax.rem(me, g)
    groups = [[o * g + i for o in range(outer)] for i in range(g)]

    wins, wouts = [], []
    for l in range(layers):
        wins.append(
            lax.all_gather(in_weight[l], "sp", axis=0, tiled=True, axis_index_groups=groups)
        )
        wouts.append(lax.all_gather(out_weight[l], "sp", axis=0, axis_index_groups=groups))

    head = taps - 1
    tail_doc = lax.ppermute(
        documents[rows - head :], "sp", [(i, i + 1) for i in range(n_sp - 1)]
    )
    tail_doc = jnp.where(me == 0, -1, tail_doc)
    ext_doc = jnp.concatenate([tail_doc, documents])
    same = [ext_doc[head - lag : head - lag + rows] == documents for lag in range(1, taps)]
    mask = jnp.stack([same[0]] + same, axis=1).astype(F32)
    mask = jnp.pad(mask, ((0, 0), (0, 128 - mask.shape[1])))

    def paired(w):
        blocks, dim = w.shape[1], w.shape[2]
        per = 128 // dim
        w = w.reshape(layers, blocks // per, per, dim, dim)
        eye = jnp.eye(per, dtype=w.dtype)
        full = w[:, :, :, :, None, :] * eye[None, None, :, None, :, None]
        return full.reshape(layers, blocks // per, per * dim, per * dim)

    gates = jnp.concatenate([paired(recur_gate), paired(input_gate)], axis=3)
    coef = -RG_C * jax.nn.softplus(-decay_param)
    vec = jnp.concatenate(
        [
            conv_taps,
            conv_bias[:, None],
            recur_bias[:, None],
            input_bias[:, None],
            coef[:, None],
        ],
        axis=1,
    )
    gain = lax.dynamic_index_in_dim(
        norm_gain.reshape(layers, outer, g, block_width), inner, 2, False
    ).reshape(layers, 1, outer * block_width)

    x = tokens.reshape(rows, outer, g, block_width).transpose(2, 0, 1, 3)
    x = swapped(x.reshape(g, rows, outer * block_width), g)
    for l in range(layers):
        x = one_layer(
            g, n_sp, n_tp, taps, x, gain[l], wins[l], wouts[l], vec[l], mask, gates[l], features
        )
    x = swapped(x, g)
    x = x.reshape(g, rows, outer, block_width).transpose(1, 2, 0, 3)
    return x.reshape(rows, features)


def solution(mesh):
    n_sp = mesh.shape["sp"]
    g = 4 if n_sp % 4 == 0 else 1
    return jax.shard_map(
        functools.partial(per_device, g),
        mesh=mesh,
        in_specs=(
            P("sp", None),
            P("sp"),
            P(),
            P(None, "sp", "tp"),
            P(None, None, "tp"),
            P(None, "tp"),
            P(None, "tp", None, None),
            P(None, "tp", None, None),
            P(None, "tp"),
            P(None, "tp"),
            P(None, "tp"),
            P(None, "tp", "sp"),
        ),
        out_specs=P("sp", None),
        check_vma=False,
    )
```

```python
import functools

import jax
import jax.numpy as jnp
from jax import lax
from jax.experimental import pallas as pl
from jax.experimental.pallas import tpu as pltpu
from jax.sharding import PartitionSpec as P

RG_C = 8.0
EPS = 0.1
MESH = pl.DeviceIdType.MESH
F32 = jnp.float32
BF16 = jnp.bfloat16
VM = pl.BlockSpec(memory_space=pltpu.VMEM)


def send(src, dst, send_sem, recv_sem, **device):
    return pltpu.make_async_remote_copy(
        src_ref=src,
        dst_ref=dst,
        send_sem=send_sem,
        recv_sem=recv_sem,
        device_id=device,
        device_id_type=MESH,
    )


def minus_expm1(x):
    series = 1.0 + x * (1.0 / 8.0)
    for n in range(7, 1, -1):
        series = 1.0 + (x * (1.0 / n)) * series
    return jnp.where(x > -0.5, -x * series, 1.0 - jnp.exp(x))


def whole_kernel(
    g, n_sp, n_tp,
    x_in, win_in, wout_in, doc_ref, gain_ref, taps_ref, bias_ref, rbias_ref, ibias_ref, coef_ref,
    rgate_ref, igate_ref,
    o_ref,
    xbuf, win, wout, part, gotten, tails, tail_out, doc_tail, docs, ext, a_buf, b_buf, ends, hid,
    psend, pgot,
    own_sem, x_send, x_recv, xt_send, xt_recv, w_send, w_recv, doc_sem, rs_send, rs_recv,
    tail_sem, end_send, end_recv, ag_send, ag_recv, tp_send, tp_recv, f_send, f_recv, ft_send,
    ft_recv,
):
    me = lax.axis_index("sp")
    core = lax.axis_index("tp")
    outer = n_sp // g
    inner, place = lax.rem(me, g), me // g
    base = place * g
    layers, width, chans = win_in.shape
    rows, features = xbuf.shape[1], xbuf.shape[2] * g
    taps = taps_ref.shape[1]
    half = rows // n_tp
    mine = pl.ds(core * half, half)
    strided = len(x_in.shape) == 2
    pieces = outer if strided else 1
    after = lax.rem(me + 1, n_sp)

    def piece(ref, at, j, o):
        if strided:
            return ref.at[at, pl.ds((o * g + j) * width, width)]
        return ref.at[j, at, :]

    def slot(ref, j, at, o):
        return ref.at[j, at, pl.ds(o * width, width)] if strided else ref.at[j, at, :]

    def weight(l, kind, o):
        if kind == 0:
            return win_in.at[l], win.at[l, pl.ds(o * width, width)]
        return wout_in.at[l], wout.at[l, o]

    line = outer == 4

    def weight_start(l, kind):
        k = 2 * l + kind
        src, dst = weight(l, kind, place)
        pltpu.make_async_copy(src, dst, own_sem.at[k]).start()
        for step in (2, 1, 3) if line else range(1, outer):
            to = lax.rem(place + step, outer)
            copy = send(src, dst, w_send.at[k, to], w_recv.at[k, place], sp=to * g + inner)
            if line:
                far = (place == 0) & (to == 3) | (place == 3) & (to == 0)
                pl.when(jnp.logical_not(far))(copy.start)
            else:
                copy.start()

    def weight_wait(l, kind, o):
        src, dst = weight(l, kind, o)
        k = 2 * l + kind
        send(src, dst, w_send.at[k, o], w_recv.at[k, o], sp=o * g + inner).wait_recv()

    def weight_relay(l, kind):
        if not line:
            return
        k = 2 * l + kind

        @pl.when((place == 1) | (place == 2))
        def _():
            o = jnp.where(place == 2, 0, 3)
            to = jnp.where(place == 2, 3, 0)
            weight_wait(l, kind, o)
            dst = weight(l, kind, o)[1]
            send(dst, dst, w_send.at[k, place], w_recv.at[k, o], sp=to * g + inner).start()

    def weight_done(l, kind):
        k = 2 * l + kind
        src, dst = weight(l, kind, place)
        pltpu.make_async_copy(src, dst, own_sem.at[k]).wait()
        for step in range(1, outer):
            o = lax.rem(place + step, outer)
            if line:
                taken = (place == 2) & (o == 0) | (place == 1) & (o == 3)
                pl.when(jnp.logical_not(taken))(functools.partial(weight_wait, l, kind, o))
            else:
                weight_wait(l, kind, o)

    def weight_close(l, kind):
        k = 2 * l + kind
        src, dst = weight(l, kind, place)
        for step in range(1, outer):
            to = lax.rem(place + step, outer)
            copy = send(src, dst, w_send.at[k, to], w_recv.at[k, place], sp=to * g + inner)
            if line:
                far = (place == 0) & (to == 3) | (place == 3) & (to == 0)
                pl.when(jnp.logical_not(far))(copy.wait_send)
            else:
                copy.wait_send()
        if line:
            copy = send(dst, dst, w_send.at[k, place], w_recv.at[k, place], sp=after)
            pl.when((place == 1) | (place == 2))(copy.wait_send)

    def x_copy(j, o, landed):
        return send(
            piece(x_in, mine, j, o),
            slot(xbuf, landed, mine, o),
            x_send.at[j, o],
            x_recv.at[landed, o],
            sp=base + j,
        )

    def x_go(step, _):
        j = lax.rem(inner + step, g)
        for o in range(pieces):
            x_copy(j, o, inner).start()
        return 0

    def own_piece(o):
        everything = pl.ds(0, rows)
        return pltpu.make_async_copy(
            piece(x_in, everything, inner, o),
            slot(xbuf, inner, everything, o),
            own_sem.at[2 * layers + o],
        )

    doc_copy = send(
        doc_ref.at[pl.ds(rows - 8, 8)], doc_tail, doc_sem.at[0], doc_sem.at[1], sp=after
    )
    weight_start(0, 0)
    lax.fori_loop(1, g, x_go, 0)
    doc_copy.start()
    for o in range(pieces):
        own_piece(o).start()

    def x_share(j, other, at):
        peer = lax.rem(core + other, n_tp)
        return send(
            xbuf.at[j, at], xbuf.at[j, at], xt_send.at[j, other - 1],
            xt_recv.at[j, n_tp - other - 1], tp=peer,
        )

    def x_arrive(step, _):
        j = lax.rem(inner + step, g)
        for o in range(pieces):
            x_copy(j, o, j).wait_recv()
        for other in range(1, n_tp):
            x_share(j, other, mine).start()
        return 0

    lax.fori_loop(1, g, x_arrive, 0)
    for o in range(pieces):
        own_piece(o).wait()
    weight_relay(0, 0)
    weight_start(0, 1)

    doc_copy.wait_recv()
    docs[pl.ds(0, 8), :] = jnp.where(me == 0, -1.0, doc_tail[...])
    docs[pl.ds(8, rows), :] = doc_ref[...]

    def x_shared(step, _):
        j = lax.rem(inner + step, g)
        for other in range(1, n_tp):
            peer = lax.rem(core + other, n_tp)
            at = pl.ds(peer * half, half)
            send(
                xbuf.at[j, at], xbuf.at[j, at], xt_send.at[j, other - 1],
                xt_recv.at[j, other - 1], tp=peer,
            ).wait_recv()
            x_share(j, other, mine).wait_send()
        for o in range(pieces):
            x_copy(j, o, inner).wait_send()
        return 0

    lax.fori_loop(1, g, x_shared, 0)
    doc_copy.wait_send()

    pair = 128
    dim = rgate_ref.shape[2]
    repeat = (
        lax.rem(lax.broadcasted_iota(jnp.int32, (dim, pair), 1), dim)
        == lax.broadcasted_iota(jnp.int32, (dim, pair), 0)
    ).astype(F32).astype(BF16)
    on_block = (
        lax.broadcasted_iota(jnp.int32, (pair, pair), 0) // dim
        == lax.broadcasted_iota(jnp.int32, (pair, pair), 1) // dim
    )

    def diagonal(ref, l, col):
        wide = jnp.dot(ref[l, pl.ds(col, pair), :], repeat, preferred_element_type=F32)
        return jnp.where(on_block, wide, 0.0).astype(BF16)

    for l in range(layers):
        last = l == layers - 1
        weight_done(l, 0)

        def project(step, _):
            j = lax.rem(inner + step, g)
            x = xbuf[j].astype(F32)
            squares = jnp.sum(x * x, axis=1, keepdims=True)
            high = squares.astype(BF16).astype(F32)
            lane = lax.broadcasted_iota(jnp.int32, (rows, 128), 1)
            extra = jnp.where(lane == 0, high, jnp.where(lane == 1, squares - high, 0.0))
            scaled = (x * gain_ref[l]).astype(BF16)
            out = jnp.dot(scaled, win[l], preferred_element_type=F32)
            part[j, :, :chans] = out.astype(BF16)
            part[j, :, chans:] = extra.astype(BF16)

            @pl.when(step < g)
            def _():
                send(
                    part.at[j], gotten.at[inner], rs_send.at[j], rs_recv.at[inner], sp=base + j
                ).start()

            return 0

        lax.fori_loop(1, g + 1, project, 0)
        ext[pl.ds(8, rows), :] = part[inner, :, :chans].astype(F32)
        sums = part[inner, :, chans:].astype(F32)

        def collect(step, sums):
            j = lax.rem(inner + step, g)
            send(part.at[j], gotten.at[j], rs_send.at[j], rs_recv.at[j], sp=base + j).wait_recv()
            ext[pl.ds(8, rows), :] += gotten[j, :, :chans].astype(F32)
            return sums + gotten[j, :, chans:].astype(F32)

        sums = lax.fori_loop(1, g, collect, sums)
        total = jnp.sum(sums, axis=1, keepdims=True)
        scale = lax.rsqrt(total * (1.0 / features) + EPS)
        mixed = (ext[pl.ds(8, rows), :] * scale).astype(BF16)
        tail_out[...] = mixed[rows - 16 :]
        tail_copy = send(
            tail_out, tails.at[l], tail_sem.at[l, 0], tail_sem.at[l, 1], sp=after
        )
        tail_copy.start()
        ext[pl.ds(8, rows), :] = mixed.astype(F32)
        weight_relay(l, 1)
        if not last:
            weight_start(l + 1, 0)
        tail_copy.wait_recv()
        ext[pl.ds(0, 8), :] = tails[l, 8:].astype(F32)

        for col in range(0, chans, pair):
            cols = pl.ds(col, pair)
            row = slice(l, l + 1)
            conv = bias_ref[row, cols] + taps_ref[l, 0:1, cols] * ext[pl.ds(8, rows), cols]
            for lag in range(1, taps):
                same = docs[pl.ds(8 - lag, rows), :] == docs[pl.ds(8, rows), :]
                shifted = ext[pl.ds(8 - lag, rows), cols]
                conv = conv + jnp.where(same, taps_ref[l, lag : lag + 1, cols] * shifted, 0.0)
            conv_out = conv.astype(BF16)
            recur = jnp.dot(conv_out, diagonal(rgate_ref, l, col), preferred_element_type=F32)
            inp = jnp.dot(conv_out, diagonal(igate_ref, l, col), preferred_element_type=F32)
            recur = jax.nn.sigmoid(recur + rbias_ref[row, cols])
            inp = jax.nn.sigmoid(inp + ibias_ref[row, cols])
            log_decay = coef_ref[row, cols] * recur
            keep = docs[pl.ds(7, rows), :] == docs[pl.ds(8, rows), :]
            a_buf[col // pair] = jnp.where(keep, jnp.exp(log_decay), 0.0)
            b_buf[col // pair] = jnp.sqrt(jnp.maximum(minus_expm1(2.0 * log_decay), 0.0)) * (
                inp * conv_out.astype(F32)
            )

        sub = rows // 8
        lanes = a_buf.shape[0]

        def advance(r, carry):
            at = pl.ds(r, 8, stride=sub)
            following = []
            for c in range(lanes):
                decay, state = carry[c]
                a = a_buf[c, at, :]
                decay = decay * a
                state = a * state + b_buf[c, at, :]
                a_buf[c, at, :] = decay
                b_buf[c, at, :] = state
                following.append((decay, state))
            return tuple(following)

        start = (jnp.ones((8, pair), F32), jnp.zeros((8, pair), F32))
        chunks = lax.fori_loop(0, sub, advance, (start,) * lanes, unroll=2)
        decay = jnp.concatenate([c[0] for c in chunks], axis=1)
        state = jnp.concatenate([c[1] for c in chunks], axis=1)
        prefix = [(jnp.ones((1, chans), F32), jnp.zeros((1, chans), F32))]
        for s in range(8):
            d, h = prefix[-1]
            prefix.append((d * decay[s : s + 1], decay[s : s + 1] * h + state[s : s + 1]))
        ends[l, me, 0:1, :] = prefix[8][0]
        ends[l, me, 1:2, :] = prefix[8][1]

        def end_copy(dst, src):
            return send(
                ends.at[l, me], ends.at[l, src], end_send.at[l, dst], end_recv.at[l, src], sp=dst
            )

        def end_to(dst, _):
            pl.when(dst > me)(lambda: end_copy(dst, me).start())
            return 0

        def end_close(dst, _):
            pl.when(dst > me)(lambda: end_copy(dst, me).wait_send())
            return 0

        def fold(src, state):
            pl.when(src < me)(lambda: end_copy(src, src).wait_recv())
            return jnp.where(src < me, ends[l, src, 0:1, :] * state + ends[l, src, 1:2, :], state)

        lax.fori_loop(0, n_sp, end_to, 0)
        carried = lax.fori_loop(0, n_sp, fold, jnp.zeros((1, chans), F32))
        for s in range(8):
            at = pl.ds(s * sub, sub)
            enter = prefix[s][0] * carried + prefix[s][1]
            for c in range(lanes):
                one = enter[:, c * pair : (c + 1) * pair]
                hid[inner, at, pl.ds(c * pair, pair)] = (
                    b_buf[c, at, :] + a_buf[c, at, :] * one
                ).astype(BF16)

        def ag_copy(j, landed):
            return send(
                hid.at[inner], hid.at[landed], ag_send.at[j], ag_recv.at[landed], sp=base + j
            )

        def spread(step, _):
            j = lax.rem(inner + step, g)
            ag_copy(j, inner).start()
            return 0

        lax.fori_loop(1, g, spread, 0)
        if not last:
            weight_relay(l + 1, 0)
            weight_start(l + 1, 1)
        weight_done(l, 1)

        def tp_copy(j, other, landed):
            peer = lax.rem(core + other, n_tp)
            return send(
                psend.at[j], pgot.at[l, landed, j], tp_send.at[other - 1, j],
                tp_recv.at[l, landed, j], tp=peer,
            )

        def unproject(step, _):
            j = lax.rem(inner + step, g)
            pl.when(step > 0)(lambda: ag_copy(j, j).wait_recv())
            h = hid[j]
            for block in range(outer):
                out = jnp.dot(h, wout[l, block], preferred_element_type=F32)
                psend[j, :, block * width : (block + 1) * width] = out.astype(BF16)
            for other in range(1, n_tp):
                tp_copy(j, other, n_tp - other - 1).start()
            return 0

        lax.fori_loop(0, g, unproject, 0)

        def f_copy(j, o, landed):
            return send(
                slot(xbuf, j, mine, o), piece(o_ref, mine, landed, o), f_send.at[j, o],
                f_recv.at[landed, o], sp=base + j,
            )

        def finish(step, _):
            j = lax.rem(inner + step, g)
            for other in range(1, n_tp):
                copy = tp_copy(j, other, other - 1)
                copy.wait_recv()
                copy.wait_send()
            at = mine if last else pl.ds(0, rows)
            summed = psend[j, at, :].astype(F32)
            for other in range(1, n_tp):
                summed = summed + pgot[l, other - 1, j, at, :].astype(F32)
            new = (xbuf[j, at, :].astype(F32) + summed).astype(BF16)
            xbuf[j, at, :] = new
            if last:

                @pl.when(step < g)
                def _():
                    for o in range(pieces):
                        f_copy(j, o, inner).start()

            return 0

        lax.fori_loop(1, g + 1, finish, 0)

        def close(step, _):
            j = lax.rem(inner + step, g)
            send(part.at[j], gotten.at[j], rs_send.at[j], rs_recv.at[j], sp=base + j).wait_send()
            ag_copy(j, j).wait_send()
            return 0

        lax.fori_loop(1, g, close, 0)
        tail_copy.wait_send()
        lax.fori_loop(0, n_sp, end_close, 0)

    for o in range(pieces):
        target = piece(o_ref, mine, inner, o)
        target[...] = slot(xbuf, inner, mine, o)[...]

    def f_arrive(step, _):
        j = lax.rem(inner + step, g)
        for o in range(pieces):
            f_copy(j, o, j).wait_recv()
        return 0

    lax.fori_loop(1, g, f_arrive, 0)

    def share_of(at):
        return o_ref.at[at] if strided else o_ref.at[:, at]

    def f_share(other, at, landed):
        return send(
            share_of(at), share_of(at), ft_send.at[other - 1], ft_recv.at[landed],
            tp=lax.rem(core + other, n_tp),
        )

    for other in range(1, n_tp):
        f_share(other, mine, n_tp - other - 1).start()
    for l in range(layers):
        weight_close(l, 0)
        weight_close(l, 1)

    def f_close(step, _):
        j = lax.rem(inner + step, g)
        for o in range(pieces):
            f_copy(j, o, inner).wait_send()
        return 0

    lax.fori_loop(1, g, f_close, 0)
    for other in range(1, n_tp):
        peer = lax.rem(core + other, n_tp)
        f_share(other, pl.ds(peer * half, half), other - 1).wait_recv()
        f_share(other, mine, other - 1).wait_send()


def per_device(
    g,
    tokens,
    documents,
    norm_gain,
    in_weight,
    conv_taps,
    conv_bias,
    recur_gate,
    input_gate,
    recur_bias,
    input_bias,
    decay_param,
    out_weight,
):
    n_sp, n_tp = lax.axis_size("sp"), lax.axis_size("tp")
    outer = n_sp // g
    rows, features = tokens.shape
    layers, width, chans = in_weight.shape
    inner = lax.rem(lax.axis_index("sp"), g)
    strided = width % 128 == 0
    pieces = outer if strided else 1
    part_width = outer * width

    docs = jnp.broadcast_to(documents.astype(F32)[:, None], (rows, 128))
    coef = -RG_C * jax.nn.softplus(-decay_param)
    gain = lax.dynamic_index_in_dim(norm_gain.reshape(layers, outer, g, width), inner, 2, False)
    gain = gain.reshape(layers, 1, part_width)
    dim = recur_gate.shape[2]
    x = tokens
    if not strided:
        x = x.reshape(rows, outer, g, width).transpose(2, 0, 1, 3).reshape(g, rows, part_width)
    dma = pltpu.SemaphoreType.DMA
    any_space = pl.BlockSpec(memory_space=pl.ANY)
    others = max(n_tp - 1, 1)
    out = pl.pallas_call(
        functools.partial(whole_kernel, g, n_sp, n_tp),
        out_shape=jax.ShapeDtypeStruct(x.shape, x.dtype),
        in_specs=[any_space] * 3 + [VM] * 9,
        out_specs=VM,
        scratch_shapes=[
            pltpu.VMEM((g, rows, part_width), BF16),
            pltpu.VMEM((layers, part_width, chans), BF16),
            pltpu.VMEM((layers, outer, chans, width), BF16),
            pltpu.VMEM((g, rows, chans + 128), BF16),
            pltpu.VMEM((g, rows, chans + 128), BF16),
            pltpu.VMEM((layers, 16, chans), BF16),
            pltpu.VMEM((16, chans), BF16),
            pltpu.VMEM((8, 128), F32),
            pltpu.VMEM((rows + 8, 128), F32),
            pltpu.VMEM((rows + 8, chans), F32),
            pltpu.VMEM((chans // 128, rows, 128), F32),
            pltpu.VMEM((chans // 128, rows, 128), F32),
            pltpu.VMEM((layers, n_sp, 2, chans), F32),
            pltpu.VMEM((g, rows, chans), BF16),
            pltpu.VMEM((g, rows, part_width), BF16),
            pltpu.VMEM((layers, others, g, rows, part_width), BF16),
            dma((2 * layers + pieces,)),
            dma((g, pieces)),
            dma((g, pieces)),
            dma((g, others)),
            dma((g, others)),
            dma((2 * layers, outer)),
            dma((2 * layers, outer)),
            dma((2,)),
            dma((g,)),
            dma((g,)),
            dma((layers, 2)),
            dma((layers, n_sp)),
            dma((layers, n_sp)),
            dma((g,)),
            dma((g,)),
            dma((others, g)),
            dma((layers, others, g)),
            dma((g, pieces)),
            dma((g, pieces)),
            dma((others,)),
            dma((others,)),
        ],
        compiler_params=pltpu.CompilerParams(
            has_side_effects=True, vmem_limit_bytes=60 * 1024 * 1024
        ),
    )(
        x, in_weight, out_weight, docs, gain, conv_taps, conv_bias, recur_bias, input_bias, coef,
        recur_gate.reshape(layers, chans, dim), input_gate.reshape(layers, chans, dim),
    )
    if not strided:
        out = out.reshape(g, rows, outer, width).transpose(1, 2, 0, 3).reshape(rows, features)
    return out


def solution(mesh):
    n_sp = mesh.shape["sp"]
    g = 4 if n_sp % 4 == 0 else 1
    return jax.shard_map(
        functools.partial(per_device, g),
        mesh=mesh,
        in_specs=(
            P("sp", None),
            P("sp"),
            P(),
            P(None, "sp", "tp"),
            P(None, None, "tp"),
            P(None, "tp"),
            P(None, "tp", None, None),
            P(None, "tp", None, None),
            P(None, "tp"),
            P(None, "tp"),
            P(None, "tp"),
            P(None, "tp", "sp"),
        ),
        out_specs=P("sp", None),
        check_vma=False,
    )
```

```python
import functools

import jax
import jax.numpy as jnp
from jax import lax
from jax.experimental import pallas as pl
from jax.experimental.pallas import tpu as pltpu
from jax.sharding import PartitionSpec as P

RG_C = 8.0
EPS = 0.1
MESH = pl.DeviceIdType.MESH
F32 = jnp.float32
BF16 = jnp.bfloat16
VM = pl.BlockSpec(memory_space=pltpu.VMEM)


def send(src, dst, send_sem, recv_sem, **device):
    return pltpu.make_async_remote_copy(
        src_ref=src,
        dst_ref=dst,
        send_sem=send_sem,
        recv_sem=recv_sem,
        device_id=device,
        device_id_type=MESH,
    )


def minus_expm1(x):
    series = 1.0 + x * (1.0 / 8.0)
    for n in range(7, 1, -1):
        series = 1.0 + (x * (1.0 / n)) * series
    return jnp.where(x > -0.5, -x * series, 1.0 - jnp.exp(x))


def whole_kernel(
    g, n_sp, n_tp,
    x_in, win_in, wout_in, doc_ref, gain_ref, taps_ref, bias_ref, rbias_ref, ibias_ref, coef_ref,
    rgate_ref, igate_ref,
    o_ref,
    xbuf, win, wout, part, gotten, tails, tail_out, doc_tail, docs, ext, a_buf, b_buf, ends, hid,
    psend, pgot,
    own_sem, x_send, x_recv, xt_send, xt_recv, w_send, w_recv, doc_sem, rs_send, rs_recv,
    tail_sem, end_send, end_recv, ag_send, ag_recv, tp_send, tp_recv, f_send, f_recv, ft_send,
    ft_recv,
):
    me = lax.axis_index("sp")
    core = lax.axis_index("tp")
    outer = n_sp // g
    inner, place = lax.rem(me, g), me // g
    base = place * g
    layers, width, chans = win_in.shape
    rows, features = xbuf.shape[1], xbuf.shape[2] * g
    taps = taps_ref.shape[1]
    halves, span = hid.shape[0], hid.shape[3]
    half = rows // n_tp
    mine = pl.ds(core * half, half)
    strided = len(x_in.shape) == 2
    pieces = outer if strided else 1
    after = lax.rem(me + 1, n_sp)

    def piece(ref, at, j, o):
        if strided:
            return ref.at[at, pl.ds((o * g + j) * width, width)]
        return ref.at[j, at, :]

    def slot(ref, j, at, o):
        return ref.at[j, at, pl.ds(o * width, width)] if strided else ref.at[j, at, :]

    def weight(l, kind, o):
        if kind == 0:
            return win_in.at[l], win.at[l, pl.ds(o * width, width)]
        return wout_in.at[l], wout.at[l, o]

    line = outer == 4

    def weight_start(l, kind):
        k = 2 * l + kind
        src, dst = weight(l, kind, place)
        pltpu.make_async_copy(src, dst, own_sem.at[k]).start()
        for step in (2, 1, 3) if line else range(1, outer):
            to = lax.rem(place + step, outer)
            copy = send(src, dst, w_send.at[k, to], w_recv.at[k, place], sp=to * g + inner)
            if line:
                far = (to - place) * (to - place) != 1
                pl.when(jnp.logical_not(far))(copy.start)
            else:
                copy.start()

    def weight_wait(l, kind, o):
        src, dst = weight(l, kind, o)
        k = 2 * l + kind
        send(src, dst, w_send.at[k, o], w_recv.at[k, o], sp=o * g + inner).wait_recv()

    def weight_relay(l, kind):
        if not line:
            return
        k = 2 * l + kind

        @pl.when((place == 1) | (place == 2))
        def _():
            for way in (1, -1):
                o, to = place - way, place + way
                weight_wait(l, kind, o)
                dst = weight(l, kind, o)[1]
                send(
                    dst, dst, w_send.at[k, outer + to], w_recv.at[k, o], sp=to * g + inner
                ).start()
            o = jnp.where(place == 2, 0, 3)
            to = jnp.where(place == 2, 3, 0)
            weight_wait(l, kind, o)
            dst = weight(l, kind, o)[1]
            send(dst, dst, w_send.at[k, place], w_recv.at[k, o], sp=to * g + inner).start()

    def weight_done(l, kind):
        k = 2 * l + kind
        src, dst = weight(l, kind, place)
        pltpu.make_async_copy(src, dst, own_sem.at[k]).wait()
        for step in range(1, outer):
            o = lax.rem(place + step, outer)
            if line:
                taken = (place == 1) | (place == 2)
                pl.when(jnp.logical_not(taken))(functools.partial(weight_wait, l, kind, o))
            else:
                weight_wait(l, kind, o)

    def weight_close(l, kind):
        k = 2 * l + kind
        src, dst = weight(l, kind, place)
        for step in range(1, outer):
            to = lax.rem(place + step, outer)
            copy = send(src, dst, w_send.at[k, to], w_recv.at[k, place], sp=to * g + inner)
            if line:
                far = (to - place) * (to - place) != 1
                pl.when(jnp.logical_not(far))(copy.wait_send)
            else:
                copy.wait_send()
        if line:
            copy = send(dst, dst, w_send.at[k, place], w_recv.at[k, place], sp=after)
            pl.when((place == 1) | (place == 2))(copy.wait_send)
            for way in (1, -1):
                at = outer + lax.rem(place + way + outer, outer)
                copy = send(dst, dst, w_send.at[k, at], w_recv.at[k, place], sp=after)
                pl.when((place == 1) | (place == 2))(copy.wait_send)

    def x_copy(j, o, landed):
        return send(
            piece(x_in, mine, j, o),
            slot(xbuf, landed, mine, o),
            x_send.at[j, o],
            x_recv.at[landed, o],
            sp=base + j,
        )

    def x_go(step, _):
        j = lax.rem(inner + step, g)
        for o in range(pieces):
            x_copy(j, o, inner).start()
        return 0

    def own_piece(o):
        everything = pl.ds(0, rows)
        return pltpu.make_async_copy(
            piece(x_in, everything, inner, o),
            slot(xbuf, inner, everything, o),
            own_sem.at[2 * layers + o],
        )

    doc_copy = send(
        doc_ref.at[pl.ds(rows - 8, 8)], doc_tail, doc_sem.at[0], doc_sem.at[1], sp=after
    )
    weight_start(0, 0)
    lax.fori_loop(1, g, x_go, 0)
    doc_copy.start()
    for o in range(pieces):
        own_piece(o).start()

    def x_share(j, other, at):
        peer = lax.rem(core + other, n_tp)
        return send(
            xbuf.at[j, at], xbuf.at[j, at], xt_send.at[j, other - 1],
            xt_recv.at[j, n_tp - other - 1], tp=peer,
        )

    def x_arrive(step, _):
        j = lax.rem(inner + step, g)
        for o in range(pieces):
            x_copy(j, o, j).wait_recv()
        for other in range(1, n_tp):
            x_share(j, other, mine).start()
        return 0

    lax.fori_loop(1, g, x_arrive, 0)
    for o in range(pieces):
        own_piece(o).wait()
    weight_relay(0, 0)
    weight_start(0, 1)

    doc_copy.wait_recv()
    docs[pl.ds(0, 8), :] = jnp.where(me == 0, -1.0, doc_tail[...])
    docs[pl.ds(8, rows), :] = doc_ref[...]

    def x_shared(step, _):
        j = lax.rem(inner + step, g)
        for other in range(1, n_tp):
            peer = lax.rem(core + other, n_tp)
            at = pl.ds(peer * half, half)
            send(
                xbuf.at[j, at], xbuf.at[j, at], xt_send.at[j, other - 1],
                xt_recv.at[j, other - 1], tp=peer,
            ).wait_recv()
            x_share(j, other, mine).wait_send()
        for o in range(pieces):
            x_copy(j, o, inner).wait_send()
        return 0

    lax.fori_loop(1, g, x_shared, 0)
    doc_copy.wait_send()

    pair = 128
    dim = rgate_ref.shape[2]
    repeat = (
        lax.rem(lax.broadcasted_iota(jnp.int32, (dim, pair), 1), dim)
        == lax.broadcasted_iota(jnp.int32, (dim, pair), 0)
    ).astype(F32).astype(BF16)
    on_block = (
        lax.broadcasted_iota(jnp.int32, (pair, pair), 0) // dim
        == lax.broadcasted_iota(jnp.int32, (pair, pair), 1) // dim
    )

    def diagonal(ref, l, col):
        wide = jnp.dot(ref[l, pl.ds(col, pair), :], repeat, preferred_element_type=F32)
        return jnp.where(on_block, wide, 0.0).astype(BF16)

    for l in range(layers):
        last = l == layers - 1
        weight_done(l, 0)

        def rs_copy(h, j, landed):
            lanes = pl.ds(0, span + 128 if h == 0 else span)
            return send(
                part.at[h, j, :, lanes], gotten.at[h, landed, :, lanes], rs_send.at[h, j],
                rs_recv.at[h, landed], sp=base + j,
            )

        for h in range(halves):

            def project(step, _):
                j = lax.rem(inner + step, g)
                if h == 0:
                    x = xbuf[j].astype(F32)
                    squares = jnp.sum(x * x, axis=1, keepdims=True)
                    high = squares.astype(BF16).astype(F32)
                    lane = lax.broadcasted_iota(jnp.int32, (rows, 128), 1)
                    extra = jnp.where(lane == 0, high, jnp.where(lane == 1, squares - high, 0.0))
                    psend[j] = (x * gain_ref[l]).astype(BF16)
                    part[0, j, :, span:] = extra.astype(BF16)
                out = jnp.dot(
                    psend[j], win[l, :, h * span : (h + 1) * span], preferred_element_type=F32
                )
                part[h, j, :, :span] = out.astype(BF16)
                pl.when(step < g)(lambda: rs_copy(h, j, inner).start())
                return 0

            lax.fori_loop(1, g + 1, project, 0)
        weight_relay(l, 1)
        if not last:
            weight_start(l + 1, 0)

        sub = rows // 8
        lanes = span // pair
        scale = None
        tail_copies, prefixes = [], []

        def end_copy(h, dst, src):
            return send(
                ends.at[l, h, me], ends.at[l, h, src], end_send.at[l, h, dst],
                end_recv.at[l, h, src], sp=dst,
            )

        for h in range(halves):
            ext[pl.ds(8, rows), :] = part[h, inner, :, :span].astype(F32)
            sums = part[0, inner, :, span:].astype(F32)

            def collect(step, sums):
                j = lax.rem(inner + step, g)
                rs_copy(h, j, j).wait_recv()
                ext[pl.ds(8, rows), :] += gotten[h, j, :, :span].astype(F32)
                return sums + gotten[0, j, :, span:].astype(F32)

            sums = lax.fori_loop(1, g, collect, sums)
            if h == 0:
                total = jnp.sum(sums, axis=1, keepdims=True)
                scale = lax.rsqrt(total * (1.0 / features) + EPS)
            mixed = (ext[pl.ds(8, rows), :] * scale).astype(BF16)
            tail_out[h] = mixed[rows - 16 :]
            tail_copy = send(
                tail_out.at[h], tails.at[l, h], tail_sem.at[l, h, 0], tail_sem.at[l, h, 1],
                sp=after,
            )
            tail_copy.start()
            tail_copies.append(tail_copy)
            ext[pl.ds(8, rows), :] = mixed.astype(F32)
            tail_copy.wait_recv()
            ext[pl.ds(0, 8), :] = tails[l, h, 8:].astype(F32)

            for c in range(lanes):
                here = pl.ds(c * pair, pair)
                col = h * span + c * pair
                cols = pl.ds(col, pair)
                at = h * lanes + c
                row = slice(l, l + 1)
                conv = bias_ref[row, cols] + taps_ref[l, 0:1, cols] * ext[pl.ds(8, rows), here]
                for lag in range(1, taps):
                    same = docs[pl.ds(8 - lag, rows), :] == docs[pl.ds(8, rows), :]
                    shifted = ext[pl.ds(8 - lag, rows), here]
                    conv = conv + jnp.where(same, taps_ref[l, lag : lag + 1, cols] * shifted, 0.0)
                conv_out = conv.astype(BF16)
                recur = jnp.dot(conv_out, diagonal(rgate_ref, l, col), preferred_element_type=F32)
                inp = jnp.dot(conv_out, diagonal(igate_ref, l, col), preferred_element_type=F32)
                recur = jax.nn.sigmoid(recur + rbias_ref[row, cols])
                inp = jax.nn.sigmoid(inp + ibias_ref[row, cols])
                log_decay = coef_ref[row, cols] * recur
                keep = docs[pl.ds(7, rows), :] == docs[pl.ds(8, rows), :]
                a_buf[at] = jnp.where(keep, jnp.exp(log_decay), 0.0)
                b_buf[at] = jnp.sqrt(jnp.maximum(minus_expm1(2.0 * log_decay), 0.0)) * (
                    inp * conv_out.astype(F32)
                )

            def advance(r, carry):
                at = pl.ds(r, 8, stride=sub)
                following = []
                for c in range(lanes):
                    decay, state = carry[c]
                    a = a_buf[h * lanes + c, at, :]
                    decay = decay * a
                    state = a * state + b_buf[h * lanes + c, at, :]
                    a_buf[h * lanes + c, at, :] = decay
                    b_buf[h * lanes + c, at, :] = state
                    following.append((decay, state))
                return tuple(following)

            start = (jnp.ones((8, pair), F32), jnp.zeros((8, pair), F32))
            chunks = lax.fori_loop(0, sub, advance, (start,) * lanes, unroll=4)
            decay = jnp.concatenate([c[0] for c in chunks], axis=1)
            state = jnp.concatenate([c[1] for c in chunks], axis=1)
            prefix = [(jnp.ones((1, span), F32), jnp.zeros((1, span), F32))]
            for s in range(8):
                d, e = prefix[-1]
                prefix.append((d * decay[s : s + 1], decay[s : s + 1] * e + state[s : s + 1]))
            prefixes.append(prefix)
            ends[l, h, me, 0:1, :] = prefix[8][0]
            ends[l, h, me, 1:2, :] = prefix[8][1]

            def end_to(dst, _):
                pl.when(dst > me)(lambda: end_copy(h, dst, me).start())
                return 0

            lax.fori_loop(0, n_sp, end_to, 0)

        if not last:
            weight_relay(l + 1, 0)
            weight_start(l + 1, 1)

        def ag_copy(h, j, landed):
            return send(
                hid.at[h, inner], hid.at[h, landed], ag_send.at[h, j], ag_recv.at[h, landed],
                sp=base + j,
            )

        for h in range(halves):

            def fold(src, state):
                pl.when(src < me)(lambda: end_copy(h, src, src).wait_recv())
                following = ends[l, h, src, 0:1, :] * state + ends[l, h, src, 1:2, :]
                return jnp.where(src < me, following, state)

            carried = lax.fori_loop(0, n_sp, fold, jnp.zeros((1, span), F32))
            for s in range(8):
                at = pl.ds(s * sub, sub)
                enter = prefixes[h][s][0] * carried + prefixes[h][s][1]
                for c in range(lanes):
                    one = enter[:, c * pair : (c + 1) * pair]
                    hid[h, inner, at, pl.ds(c * pair, pair)] = (
                        b_buf[h * lanes + c, at, :] + a_buf[h * lanes + c, at, :] * one
                    ).astype(BF16)

            def spread(step, _):
                j = lax.rem(inner + step, g)
                ag_copy(h, j, inner).start()
                return 0

            lax.fori_loop(1, g, spread, 0)
        weight_done(l, 1)

        def tp_copy(j, other, landed):
            peer = lax.rem(core + other, n_tp)
            return send(
                psend.at[j], pgot.at[l, landed, j], tp_send.at[other - 1, j],
                tp_recv.at[l, landed, j], tp=peer,
            )

        def unproject(step, _):
            j = lax.rem(inner + step, g)
            for h in range(halves):
                pl.when(step > 0)(lambda: ag_copy(h, j, j).wait_recv())
            for block in range(outer):
                out = 0.0
                for h in range(halves):
                    out = out + jnp.dot(
                        hid[h, j], wout[l, block, h * span : (h + 1) * span],
                        preferred_element_type=F32,
                    )
                psend[j, :, block * width : (block + 1) * width] = out.astype(BF16)
            for other in range(1, n_tp):
                tp_copy(j, other, n_tp - other - 1).start()
            return 0

        lax.fori_loop(0, g, unproject, 0)

        def f_copy(j, o, landed):
            return send(
                slot(xbuf, j, mine, o), piece(o_ref, mine, landed, o), f_send.at[j, o],
                f_recv.at[landed, o], sp=base + j,
            )

        def finish(step, _):
            j = lax.rem(inner + step, g)
            for other in range(1, n_tp):
                copy = tp_copy(j, other, other - 1)
                copy.wait_recv()
                copy.wait_send()
            at = mine if last else pl.ds(0, rows)
            summed = psend[j, at, :].astype(F32)
            for other in range(1, n_tp):
                summed = summed + pgot[l, other - 1, j, at, :].astype(F32)
            new = (xbuf[j, at, :].astype(F32) + summed).astype(BF16)
            xbuf[j, at, :] = new
            if last:

                @pl.when(step < g)
                def _():
                    for o in range(pieces):
                        f_copy(j, o, inner).start()

            return 0

        lax.fori_loop(1, g + 1, finish, 0)

        def close(step, _):
            j = lax.rem(inner + step, g)
            for h in range(halves):
                rs_copy(h, j, j).wait_send()
                ag_copy(h, j, j).wait_send()
            return 0

        lax.fori_loop(1, g, close, 0)

        def end_close(dst, _):
            for h in range(halves):
                pl.when(dst > me)(lambda: end_copy(h, dst, me).wait_send())
            return 0

        lax.fori_loop(0, n_sp, end_close, 0)
        for tail_copy in tail_copies:
            tail_copy.wait_send()

    for o in range(pieces):
        target = piece(o_ref, mine, inner, o)
        target[...] = slot(xbuf, inner, mine, o)[...]

    def f_arrive(step, _):
        j = lax.rem(inner + step, g)
        for o in range(pieces):
            f_copy(j, o, j).wait_recv()
        return 0

    lax.fori_loop(1, g, f_arrive, 0)

    def share_of(at):
        return o_ref.at[at] if strided else o_ref.at[:, at]

    def f_share(other, at, landed):
        return send(
            share_of(at), share_of(at), ft_send.at[other - 1], ft_recv.at[landed],
            tp=lax.rem(core + other, n_tp),
        )

    for other in range(1, n_tp):
        f_share(other, mine, n_tp - other - 1).start()
    for l in range(layers):
        weight_close(l, 0)
        weight_close(l, 1)

    def f_close(step, _):
        j = lax.rem(inner + step, g)
        for o in range(pieces):
            f_copy(j, o, inner).wait_send()
        return 0

    lax.fori_loop(1, g, f_close, 0)
    for other in range(1, n_tp):
        peer = lax.rem(core + other, n_tp)
        f_share(other, pl.ds(peer * half, half), other - 1).wait_recv()
        f_share(other, mine, other - 1).wait_send()


def per_device(
    g,
    tokens,
    documents,
    norm_gain,
    in_weight,
    conv_taps,
    conv_bias,
    recur_gate,
    input_gate,
    recur_bias,
    input_bias,
    decay_param,
    out_weight,
):
    n_sp, n_tp = lax.axis_size("sp"), lax.axis_size("tp")
    outer = n_sp // g
    rows, features = tokens.shape
    layers, width, chans = in_weight.shape
    inner = lax.rem(lax.axis_index("sp"), g)
    strided = width % 128 == 0
    pieces = outer if strided else 1
    part_width = outer * width
    halves = 2 if chans % 256 == 0 else 1
    span = chans // halves

    docs = jnp.broadcast_to(documents.astype(F32)[:, None], (rows, 128))
    coef = -RG_C * jax.nn.softplus(-decay_param)
    gain = lax.dynamic_index_in_dim(norm_gain.reshape(layers, outer, g, width), inner, 2, False)
    gain = gain.reshape(layers, 1, part_width)
    dim = recur_gate.shape[2]
    x = tokens
    if not strided:
        x = x.reshape(rows, outer, g, width).transpose(2, 0, 1, 3).reshape(g, rows, part_width)
    dma = pltpu.SemaphoreType.DMA
    any_space = pl.BlockSpec(memory_space=pl.ANY)
    others = max(n_tp - 1, 1)
    out = pl.pallas_call(
        functools.partial(whole_kernel, g, n_sp, n_tp),
        out_shape=jax.ShapeDtypeStruct(x.shape, x.dtype),
        in_specs=[any_space] * 3 + [VM] * 9,
        out_specs=VM,
        scratch_shapes=[
            pltpu.VMEM((g, rows, part_width), BF16),
            pltpu.VMEM((layers, part_width, chans), BF16),
            pltpu.VMEM((layers, outer, chans, width), BF16),
            pltpu.VMEM((halves, g, rows, span + 128), BF16),
            pltpu.VMEM((halves, g, rows, span + 128), BF16),
            pltpu.VMEM((layers, halves, 16, span), BF16),
            pltpu.VMEM((halves, 16, span), BF16),
            pltpu.VMEM((8, 128), F32),
            pltpu.VMEM((rows + 8, 128), F32),
            pltpu.VMEM((rows + 8, span), F32),
            pltpu.VMEM((chans // 128, rows, 128), F32),
            pltpu.VMEM((chans // 128, rows, 128), F32),
            pltpu.VMEM((layers, halves, n_sp, 2, span), F32),
            pltpu.VMEM((halves, g, rows, span), BF16),
            pltpu.VMEM((g, rows, part_width), BF16),
            pltpu.VMEM((layers, others, g, rows, part_width), BF16),
            dma((2 * layers + pieces,)),
            dma((g, pieces)),
            dma((g, pieces)),
            dma((g, others)),
            dma((g, others)),
            dma((2 * layers, 2 * outer)),
            dma((2 * layers, 2 * outer)),
            dma((2,)),
            dma((halves, g)),
            dma((halves, g)),
            dma((layers, halves, 2)),
            dma((layers, halves, n_sp)),
            dma((layers, halves, n_sp)),
            dma((halves, g)),
            dma((halves, g)),
            dma((others, g)),
            dma((layers, others, g)),
            dma((g, pieces)),
            dma((g, pieces)),
            dma((others,)),
            dma((others,)),
        ],
        compiler_params=pltpu.CompilerParams(
            has_side_effects=True, vmem_limit_bytes=60 * 1024 * 1024
        ),
    )(
        x, in_weight, out_weight, docs, gain, conv_taps, conv_bias, recur_bias, input_bias, coef,
        recur_gate.reshape(layers, chans, dim), input_gate.reshape(layers, chans, dim),
    )
    if not strided:
        out = out.reshape(g, rows, outer, width).transpose(1, 2, 0, 3).reshape(rows, features)
    return out


def solution(mesh):
    n_sp = mesh.shape["sp"]
    g = 4 if n_sp % 4 == 0 else 1
    return jax.shard_map(
        functools.partial(per_device, g),
        mesh=mesh,
        in_specs=(
            P("sp", None),
            P("sp"),
            P(),
            P(None, "sp", "tp"),
            P(None, None, "tp"),
            P(None, "tp"),
            P(None, "tp", None, None),
            P(None, "tp", None, None),
            P(None, "tp"),
            P(None, "tp"),
            P(None, "tp"),
            P(None, "tp", "sp"),
        ),
        out_specs=P("sp", None),
        check_vma=False,
    )
```
